512 devices in a mesh: sp: 16 (over z), tp: 32 (over y, x, core).
Axes of the slice: x: 4, y: 4, z: 16, core: 2. Of those that a mesh axis runs over, the one named last changes fastest.
Arguments:
- latent: bfloat16 [8192, 4096], P(('sp', 'tp')), may hold values from -6 to 6
- context: bfloat16 [512, 4096], P('sp'), may hold values from -6 to 6
- condition: float32 [4096], P('sp'), may hold values from -6 to 6
- context_cond: float32 [4096], P('sp'), may hold values from -6 to 6
- mod_weight: bfloat16 [4096, 12288], P('sp', 'tp'), may hold values from -0.09375 to 0.09375
- norm_gain: float32 [4096], replicated, may hold values from 0.1 to 1.9
- query_weight: bfloat16 [4096, 4096], P(None, 'tp'), may hold values from -0.09375 to 0.09375
- key_weight: bfloat16 [4096, 2048], P(None, 'tp'), may hold values from -0.09375 to 0.09375
- value_weight: bfloat16 [4096, 2048], P(None, 'tp'), may hold values from -0.09375 to 0.09375
- out_weight: bfloat16 [4096, 4096], P(None, 'tp'), may hold values from -0.375 to 0.375
- query_gain: float32 [64], replicated, may hold values from 1.2 to 6
- key_gain: float32 [64], replicated, may hold values from 1.2 to 6
- context_lift: float32 [64], P('tp'), may hold values from 0.5 to 2
Outputs:
- updated: bfloat16 [8192, 4096], P(('sp', 'tp'))
The draws below stay inside these ranges and needn't reach their ends.
All inputs are finite; a program needn't handle non-finite values.
Results may differ from the reference program's by a relative error of at most 0.0085.
The reference program's roundings to bfloat16 on the way count: a program that leaves them out, or rounds other values in their place, can miss the bound.
Values may be sent and summed in bfloat16 or wider, within the bound.
No kernel may reach another device: no remote copies, remote signals or barrier semaphores. Data moves between devices by JAX's collectives and lax.ppermute only.
A program may use at most 64 MiB of HBM per device.

```python
import math
import jax
import jax.numpy as jnp
from jax import lax

D = 4096
HD = 64
Q_HEADS = 64
KV_HEADS = 32
GRID_W = 64
CTX = 512
SEQ = 8192


def draw_query_gain(key, part):
    subkey = jax.random.fold_in(key, 101)
    return jax.random.uniform(subkey, (HD,), jnp.float32, 1.2, 2.0)


def draw_key_gain(key, part):
    subkey = jax.random.fold_in(key, 202)
    return jax.random.uniform(subkey, (HD,), jnp.float32, 1.2, 2.0)


def block_scale(rng, dims, split, low, largest):
    level, own = 1.0, jax.random.fold_in(rng, 6)
    for position, shards_of in split:
        draws = jnp.exp(jax.random.uniform(jax.random.fold_in(own, position), (shards_of,), jnp.float32, low / len(split), largest / len(split)))
        level = level * jnp.repeat(draws, dims[position] // shards_of).reshape([-1 if axis == position else 1 for axis in range(len(dims))])
    return level


def normal_values(rng, dims, spread, reach, pieces=(), kind=jnp.bfloat16):
    result = spread * jax.random.normal(rng, dims, jnp.float32)
    if pieces:
        result = result * block_scale(rng, dims, pieces, -0.22, 0.18)
    return jnp.clip(result, -reach, reach).astype(kind)


def setup_inputs(seed: int = 0) -> dict:
    seeds = jax.random.split(jax.random.key(seed), 14)
    latent = normal_values(seeds[0], (SEQ, D), 1.0, 6.0, ((0, 512),))
    context = normal_values(seeds[1], (CTX, D), 1.0, 6.0, ((0, 16),))
    condition = normal_values(seeds[2], (D,), 1.0, 6.0, ((0, 16),), jnp.float32)
    context_cond = normal_values(seeds[3], (D,), 1.0, 6.0, ((0, 16),), jnp.float32)
    mod_weight = normal_values(seeds[4], (D, 3 * D), D ** -0.5, 0.09375, ((0, 16), (1, 32)))
    norm_gain = jnp.clip(1.0 + 0.18 * jax.random.normal(seeds[5], (D,), jnp.float32), 0.1, 1.9)
    query_weight = normal_values(seeds[6], (D, Q_HEADS * HD), D ** -0.5, 0.09375, ((1, 32),))
    key_weight = normal_values(seeds[7], (D, KV_HEADS * HD), D ** -0.5, 0.09375, ((1, 32),))
    value_weight = normal_values(seeds[8], (D, KV_HEADS * HD), D ** -0.5, 0.09375, ((1, 32),))
    out_weight = normal_values(seeds[9], (Q_HEADS * HD, D), (Q_HEADS * HD // 16) ** -0.5, 0.375, ((1, 32),))
    query_gain = draw_query_gain(jax.random.fold_in(seeds[13], 71), 0)
    key_gain = draw_key_gain(jax.random.fold_in(seeds[13], 71), 0)
    context_lift = jnp.clip(0.5 + 1.5 * jax.random.uniform(seeds[12], (Q_HEADS,), jnp.float32) ** block_scale(seeds[12], (Q_HEADS,), ((0, 32),), -0.2, 0.2), 0.5, 2.0)
    return {"latent": latent, "context": context, "condition": condition, "context_cond": context_cond, "mod_weight": mod_weight, "norm_gain": norm_gain, "query_weight": query_weight, "key_weight": key_weight, "value_weight": value_weight, "out_weight": out_weight, "query_gain": query_gain, "key_gain": key_gain, "context_lift": context_lift}


EPS = 1e-06

def modulate(row_block, gain_vec, mod_row, model_width):
    row_values = row_block.astype(jnp.float32)
    normal = row_values * lax.rsqrt(lax.optimization_barrier(jnp.mean(row_values * row_values, axis=-1, keepdims=True)) + EPS)
    shift_part = mod_row[:model_width]
    scale_part = mod_row[model_width:2 * model_width]
    return (normal * gain_vec * (1.0 + scale_part) + shift_part).astype(jnp.bfloat16)

def head_norm(values, gain_vec):
    return values * lax.rsqrt(lax.optimization_barrier(jnp.mean(values * values, axis=-1, keepdims=True)) + EPS) * gain_vec

def rope_tables(positions, head_size):
    freq_count = head_size // 4
    inverse = 10000.0 ** (-jnp.arange(freq_count, dtype=jnp.float32) / freq_count)
    grid_row = (positions // GRID_W).astype(jnp.float32)
    grid_col = (positions % GRID_W).astype(jnp.float32)
    angles = jnp.concatenate([grid_row[:, None] * inverse, grid_col[:, None] * inverse], axis=-1)
    return (jnp.cos(angles), jnp.sin(angles))

def rotate(values, cos_table, sin_table):
    paired = values.reshape(values.shape[:-1] + (values.shape[-1] // 2, 2))
    even_part = paired[..., 0]
    odd_part = paired[..., 1]
    cos_wide = cos_table[:, None, :]
    sin_wide = sin_table[:, None, :]
    turned = jnp.stack([even_part * cos_wide - odd_part * sin_wide, even_part * sin_wide + odd_part * cos_wide], axis=-1)
    return turned.reshape(values.shape)

def reference(latent, context, condition, context_cond, mod_weight, norm_gain, query_weight, key_weight, value_weight, out_weight, query_gain, key_gain, context_lift):
    model_width = latent.shape[1]
    cond_pair = jax.nn.silu(jnp.stack([condition, context_cond]).astype(jnp.float32)).astype(jnp.bfloat16)
    modulation = jnp.dot(cond_pair, mod_weight, preferred_element_type=jnp.float32)
    normed = modulate(latent, norm_gain, modulation[0], model_width)
    normed_ctx = modulate(context, norm_gain, modulation[1], model_width)
    positions = jnp.arange(SEQ, dtype=jnp.int32)
    cos_table, sin_table = rope_tables(positions, HD)
    query_raw = jnp.dot(normed, query_weight, preferred_element_type=jnp.float32).reshape(SEQ, Q_HEADS, HD)
    queries = rotate(head_norm(query_raw, query_gain), cos_table, sin_table).astype(jnp.bfloat16)
    key_raw = jnp.dot(normed, key_weight, preferred_element_type=jnp.float32).reshape(SEQ, KV_HEADS, HD)
    keys = rotate(head_norm(key_raw, key_gain), cos_table, sin_table).astype(jnp.bfloat16)
    values = jnp.dot(normed, value_weight, preferred_element_type=jnp.float32).astype(jnp.bfloat16)
    ctx_raw = jnp.dot(normed_ctx, key_weight, preferred_element_type=jnp.float32).reshape(CTX, KV_HEADS, HD)
    ctx_keys = head_norm(ctx_raw, key_gain).astype(jnp.bfloat16)
    ctx_values = jnp.dot(normed_ctx, value_weight, preferred_element_type=jnp.float32).astype(jnp.bfloat16)
    group_size = Q_HEADS // KV_HEADS
    score_scale = HD ** (-0.5)
    query_heads = queries.reshape(SEQ, KV_HEADS, group_size, HD).transpose(1, 0, 2, 3)
    key_heads = keys.transpose(1, 0, 2)
    value_heads = values.reshape(SEQ, KV_HEADS, HD).transpose(1, 0, 2)
    ctx_key_heads = ctx_keys.transpose(1, 0, 2)
    ctx_value_heads = ctx_values.reshape(CTX, KV_HEADS, HD).transpose(1, 0, 2)
    lift_rows = context_lift.reshape(KV_HEADS, group_size)
    query_block = math.gcd(SEQ, 512)

    def per_head(inputs):
        q_head, k_head, v_head, ck_head, cv_head, lift_row = inputs
        k_wide = k_head.astype(jnp.float32)
        v_wide = v_head.astype(jnp.float32)
        ck_wide = ck_head.astype(jnp.float32)
        cv_wide = cv_head.astype(jnp.float32)
        blocks = q_head.reshape(SEQ // query_block, query_block, group_size, HD)

        def per_block(q_block):
            q_wide = q_block.astype(jnp.float32)
            lat_scores = jnp.einsum('qgd,kd->gqk', q_wide, k_wide) * score_scale
            ctx_scores = jnp.einsum('qgd,kd->gqk', q_wide, ck_wide) * score_scale + lift_row[:, None, None]
            peak = jnp.maximum(lax.optimization_barrier(jnp.max(lat_scores, axis=-1)), lax.optimization_barrier(jnp.max(ctx_scores, axis=-1)))[..., None]
            lat_expo = jnp.exp(lat_scores - peak)
            ctx_expo = jnp.exp(ctx_scores - peak)
            denom = lax.optimization_barrier(jnp.sum(lat_expo, axis=-1)) + lax.optimization_barrier(jnp.sum(ctx_expo, axis=-1))
            lat_probs = lax.optimization_barrier(lat_expo.astype(jnp.bfloat16)).astype(jnp.float32)
            ctx_probs = lax.optimization_barrier(ctx_expo.astype(jnp.bfloat16)).astype(jnp.float32)
            numer = jnp.einsum('gqk,kd->gqd', lat_probs, v_wide) + jnp.einsum('gqk,kd->gqd', ctx_probs, cv_wide)
            return (numer / denom[..., None]).astype(jnp.bfloat16)
        return lax.map(per_block, blocks)
    heads_out = lax.map(per_head, (query_heads, key_heads, value_heads, ctx_key_heads, ctx_value_heads, lift_rows))
    attended = heads_out.transpose(1, 3, 0, 2, 4).reshape(SEQ, Q_HEADS * HD)
    mixed = jnp.dot(attended, out_weight, preferred_element_type=jnp.float32).astype(jnp.bfloat16)
    gate_lat = modulation[0, 2 * model_width:]
    return (latent.astype(jnp.float32) + gate_lat * mixed.astype(jnp.float32)).astype(jnp.bfloat16)
```

```python
import functools
import math
import jax
import jax.numpy as jnp
from jax import lax
from jax.experimental import pallas as pl
from jax.experimental.pallas import tpu as pltpu
from jax.sharding import PartitionSpec as P

GRID_W = 64
EPS = 1e-06
LOG2E = math.log2(math.e)
NY = 4
NX = 4
NXC = 8


def copy_for_each(shard, axis):
    copies = jnp.broadcast_to(shard, (lax.axis_size(axis), *shard.shape))
    return lax.all_to_all(copies, axis, split_axis=0, concat_axis=0, tiled=True)


def modulated(x, gain, shift):
    x = x.astype(jnp.float32)
    ms = jnp.mean(x * x, axis=-1, keepdims=True)
    return (x * lax.rsqrt(ms + EPS) * gain + shift).astype(jnp.bfloat16)


def qkv_body(hs, lat_ref, ctx_ref, gain_ref, shift_ref, w_ref, w2_ref, qg_ref, kg_ref, cos_ref, sin_ref, own_ref, other_ref, ctx_kv_ref):
    def unit(v):
        return v * lax.rsqrt(jnp.mean(v * v, axis=-1, keepdims=True) + EPS)

    def turn(v, cos, sin):
        lane = lax.broadcasted_iota(jnp.int32, v.shape, 1)
        left = pltpu.roll(v, v.shape[1] - 1, 1)
        right = pltpu.roll(v, 1, 1)
        return v * cos + jnp.where(lane % 2 == 0, left, right) * sin

    x = modulated(lat_ref[...], gain_ref[0:1], shift_ref[0:1])
    cos = cos_ref[...]
    sin = sin_ref[...]
    for w, o_ref in ((w_ref, own_ref), (w2_ref, other_ref)):
        y = jnp.dot(x, w[...], preferred_element_type=jnp.float32)
        q = jnp.concatenate([unit(y[:, :hs]), unit(y[:, hs : 2 * hs])], axis=1) * qg_ref[...]
        q = turn(q, cos, sin).astype(jnp.bfloat16)
        o_ref[:, : 2 * hs] = q * jnp.bfloat16(hs ** -0.5)
        kv = y[:, 2 * hs :]
        k = unit(kv[:, :hs]) * kg_ref[...]
        k2 = turn(jnp.concatenate([k, k], axis=1), cos, sin)
        lane = lax.broadcasted_iota(jnp.int32, k2.shape, 1)
        o_ref[:, 2 * hs :] = jnp.where(lane < hs, k2, kv).astype(jnp.bfloat16)

    @pl.when(pl.program_id(0) == 0)
    def _():
        c = modulated(ctx_ref[...], gain_ref[1:2], shift_ref[1:2])
        ckv = jnp.dot(c, w_ref[:, 2 * hs :], preferred_element_type=jnp.float32)
        ck = unit(ckv[:, :hs]) * kg_ref[...]
        ctx_kv_ref[...] = jnp.concatenate([ck, ckv[:, hs:]], axis=1).astype(jnp.bfloat16)


def qkv(lat, context, gain, shift, w, w2, qg, kg, cos, sin):
    rows, width = lat.shape
    n_ctx = context.shape[0]
    hs = kg.shape[1]
    step = rows // 2
    whole = lambda a: pl.BlockSpec(a.shape, lambda i: (0,) * a.ndim)
    return pl.pallas_call(
        functools.partial(qkv_body, hs),
        grid=(rows // step,),
        in_specs=[
            pl.BlockSpec((step, width), lambda i: (i, 0)),
            whole(context), whole(gain), whole(shift), whole(w), whole(w2), whole(qg), whole(kg),
            pl.BlockSpec((step, 2 * hs), lambda i: (i, 0)),
            pl.BlockSpec((step, 2 * hs), lambda i: (i, 0)),
        ],
        out_specs=[
            pl.BlockSpec((step, 4 * hs), lambda i: (i, 0)),
            pl.BlockSpec((step, 4 * hs), lambda i: (i, 0)),
            pl.BlockSpec((n_ctx, 2 * hs), lambda i: (0, 0)),
        ],
        out_shape=[
            jax.ShapeDtypeStruct((rows, 4 * hs), jnp.bfloat16),
            jax.ShapeDtypeStruct((rows, 4 * hs), jnp.bfloat16),
            jax.ShapeDtypeStruct((n_ctx, 2 * hs), jnp.bfloat16),
        ],
        cost_estimate=pl.CostEstimate(flops=4 * rows * width * 4 * hs, bytes_accessed=6 << 20, transcendentals=0),
        name="qkv",
    )(lat, context, gain, shift, w, w2, qg, kg, cos, sin)


def assemble_body(core_ref, own_ref, got_ref, ctx_ref, qt_ref, kv_ref):
    rows = own_ref.shape[0]
    hs = qt_ref.shape[1]

    def put(ref, start):
        t = ref[:, : 2 * hs].astype(jnp.float32).T.astype(jnp.bfloat16)
        qt_ref[0, :, start : start + rows] = t[:hs]
        qt_ref[1, :, start : start + rows] = t[hs:]

    @pl.when(core_ref[0] == 0)
    def _():
        put(own_ref, 0)
        put(got_ref, rows)

    @pl.when(core_ref[0] != 0)
    def _():
        put(got_ref, 0)
        put(own_ref, rows)

    kv_ref[0:rows] = own_ref[:, 2 * hs :]
    kv_ref[rows : 2 * rows] = got_ref[:, 2 * hs :]
    kv_ref[2 * rows :] = ctx_ref[...]


VMEM = pl.BlockSpec(memory_space=pltpu.VMEM)


def assemble(core, own, got, ctx_kv):
    rows, cols = own.shape
    hs = cols // 4
    return pl.pallas_call(
        assemble_body,
        in_specs=[pl.BlockSpec(memory_space=pltpu.SMEM), VMEM, VMEM, VMEM],
        out_specs=[VMEM, VMEM],
        out_shape=[
            pltpu.VMEM((2, hs, 2 * rows), jnp.bfloat16),
            pltpu.VMEM((2 * rows + ctx_kv.shape[0], 2 * hs), jnp.bfloat16),
        ],
        name="assemble",
    )(core, own, got, ctx_kv)


def flash_body(n_blocks, first, last, lat_rows, hs, *refs):
    qt_ref, lift_ref = refs[:2]
    blocks = refs[2 : 2 + n_blocks]
    rest = refs[2 + n_blocks :]
    if not first:
        m_ref, l_ref, acc_ref = rest[:3]
        rest = rest[3:]
    heads, _, qn = qt_ref.shape
    lift = lift_ref[...]
    for h in range(heads):
        parts = []
        top = None
        for b in blocks:
            s = jnp.dot(b[:, :hs], qt_ref[h], preferred_element_type=jnp.float32) * LOG2E
            c = s[lat_rows:] + lift[h : h + 1] * LOG2E
            s = s[:lat_rows]
            t = jnp.maximum(jnp.max(s, axis=0, keepdims=True), jnp.max(c, axis=0, keepdims=True))
            top = t if top is None else jnp.maximum(top, t)
            parts.append((b, s, c))
        if first:
            l = jnp.zeros_like(top)
            acc = jnp.zeros((hs, qn), jnp.float32)
        else:
            m = m_ref[h : h + 1]
            top = jnp.maximum(top, m)
            alpha = jnp.exp2(m - top)
            l = l_ref[h : h + 1] * alpha
            acc = acc_ref[h] * alpha
        for b, s, c in parts:
            e = jnp.exp2(s - top)
            f = jnp.exp2(c - top)
            l = l + (jnp.sum(e, axis=0, keepdims=True) + jnp.sum(f, axis=0, keepdims=True))
            p = jnp.concatenate([e.astype(jnp.bfloat16), f.astype(jnp.bfloat16)], axis=0)
            acc = acc + lax.dot_general(
                b[:, hs:], p, (((0,), (0,)), ((), ())), preferred_element_type=jnp.float32
            )
        if last:
            o = (acc / l).T.astype(jnp.bfloat16)
            n = lat_rows // (2 * NY)
            for c2 in range(2):
                for y in range(NY):
                    j = (c2 * NY + y) * n
                    rest[0][y, c2 * n : (c2 + 1) * n, h * hs : (h + 1) * hs] = o[j : j + n]
        else:
            rest[0][h : h + 1] = top
            rest[1][h : h + 1] = l
            rest[2][h] = acc


def flash(qt, lift, blocks, state, lat_rows, last):
    heads, hs, qn = qt.shape
    first = state is None
    args = [qt, lift, *blocks] + ([] if first else list(state))
    args = [pltpu.with_memory_space_constraint(a, pltpu.VMEM) for a in args]
    if last:
        outs = [pltpu.VMEM((NY, qn // NY, heads * hs), jnp.bfloat16)]
    else:
        outs = [
            pltpu.VMEM((heads, qn), jnp.float32),
            pltpu.VMEM((heads, qn), jnp.float32),
            pltpu.VMEM((heads, hs, qn), jnp.float32),
        ]
    res = pl.pallas_call(
        functools.partial(flash_body, len(blocks), first, last, lat_rows, hs),
        in_specs=[VMEM] * len(args),
        out_specs=[VMEM] * len(outs),
        out_shape=outs,
        cost_estimate=pl.CostEstimate(
            flops=4 * heads * hs * qn * blocks[0].shape[0] * len(blocks), bytes_accessed=1 << 20, transcendentals=0
        ),
        name="flash",
    )(*args)
    return res[0] if last else res


def project_body(a_ref, w_ref, o_ref):
    ny = a_ref.shape[0]
    a = jnp.concatenate([a_ref[y] for y in range(ny)], axis=1)
    n = w_ref.shape[4]

    def column(j):
        return jnp.concatenate([w_ref[0, j, y] for y in range(ny)], axis=0)

    for j in range(0, w_ref.shape[1], 2):
        w = jnp.concatenate([column(j), column(j + 1)], axis=1)
        o_ref[:, j * n : (j + 2) * n] = jnp.dot(a, w, preferred_element_type=jnp.float32).astype(jnp.bfloat16)


def out_partial(a, w):
    ny, nxc, ny2, kk, n = w.shape
    rows = a.shape[1]
    return pl.pallas_call(
        project_body,
        grid=(ny,),
        in_specs=[
            pl.BlockSpec(a.shape, lambda i: (0, 0, 0)),
            pl.BlockSpec((1, nxc, ny2, kk, n), lambda i: (i, 0, 0, 0, 0)),
        ],
        out_specs=pl.BlockSpec((rows, nxc * n), lambda i: (0, i)),
        out_shape=jax.ShapeDtypeStruct((rows, ny * nxc * n), jnp.bfloat16),
        cost_estimate=pl.CostEstimate(flops=2 * rows * w.size, bytes_accessed=2 * w.size, transcendentals=0),
        name="out_partial",
    )(a, w)


def local(
    latent,
    context,
    condition,
    context_cond,
    mod_weight,
    norm_gain,
    query_weight,
    key_weight,
    value_weight,
    out_weight,
    query_gain,
    key_gain,
    context_lift,
):
    own_rows, width = latent.shape
    hs = query_gain.shape[0]
    n_sp = lax.axis_size("sp")
    n_tp = lax.axis_size("tp")
    group_y = [[y * NXC + c for y in range(NY)] for c in range(NXC)]
    group_cx = [[y * NXC + 2 * x + c for c in range(2) for x in range(NX)] for y in range(NY)]
    group_core = [[2 * i + c for i in range(n_tp // 2)] for c in range(2)]
    swap = [(t, t ^ 1) for t in range(n_tp)]
    tp = lax.axis_index("tp")
    core = tp % 2
    block_rows = own_rows * n_tp

    lat_copies = jnp.broadcast_to(latent, (n_tp // 2, own_rows, width))
    lat_half = lax.all_to_all(lat_copies, "tp", 0, 0, axis_index_groups=group_core, tiled=True)
    lat_half = lat_half.reshape(block_rows // 2, width)

    half = jnp.arange(block_rows // 2, dtype=jnp.int32)
    inside = (half // own_rows) * (2 * own_rows) + core * own_rows + half % own_rows
    positions = lax.axis_index("sp") * block_rows + inside
    freq_count = hs // 4
    inverse = 10000.0 ** (-jnp.arange(freq_count, dtype=jnp.float32) / freq_count)
    grid_row = (positions // GRID_W).astype(jnp.float32)
    grid_col = (positions % GRID_W).astype(jnp.float32)
    angles = jnp.concatenate([grid_row[:, None] * inverse, grid_col[:, None] * inverse], axis=-1)
    cos = jnp.tile(jnp.repeat(jnp.cos(angles), 2, axis=1), (1, 2))
    sign = jnp.tile(jnp.array([-1.0, 1.0], jnp.float32), hs)
    sin = jnp.tile(jnp.repeat(jnp.sin(angles), 2, axis=1), (1, 2)) * sign
    w_own = jnp.concatenate([query_weight, key_weight, value_weight], axis=1)
    w_other = lax.ppermute(w_own, "tp", swap)
    per_head = out_weight.shape[0] // n_tp
    w_split = out_weight.reshape(NY, NXC, per_head, out_weight.shape[1]).transpose(1, 0, 2, 3)
    w_split = jnp.broadcast_to(w_split, (NY, *w_split.shape)).reshape(n_tp, *w_split.shape[1:])
    lift = jnp.broadcast_to(context_lift[:, None], (context_lift.shape[0], block_rows))
    q_gain = jnp.tile(query_gain, 2)[None]
    k_gain = key_gain[None]

    cond_pair = jax.nn.silu(jnp.stack([condition, context_cond])).astype(jnp.bfloat16)
    partial_mod = jnp.dot(cond_pair, mod_weight, preferred_element_type=jnp.float32)
    summed_mod = lax.psum(partial_mod, "sp")
    summed_mod, lat_half, w_own, cos, sin, w_split, lift, q_gain, k_gain = lax.optimization_barrier(
        (summed_mod, lat_half, w_own, cos, sin, w_split, lift, q_gain, k_gain)
    )
    mod = copy_for_each(summed_mod, "tp")
    mod = jnp.moveaxis(mod, 0, 1).reshape(2, 3 * width)
    shift = mod[:, :width]
    gain = norm_gain * (1.0 + mod[:, width : 2 * width])

    own, other, ctx_kv = qkv(lat_half, context, gain, shift, w_own, w_other, q_gain, k_gain, cos, sin)
    got = lax.ppermute(other, "tp", swap)
    qt, kv = assemble(core.reshape(1).astype(jnp.int32), own, got, ctx_kv)
    kv, w_split = lax.optimization_barrier((kv, w_split))
    w_rows = lax.all_to_all(w_split, "tp", 0, 0, tiled=True)

    up = [(i, (i + 1) % n_sp) for i in range(n_sp)]
    down = [(d, s) for s, d in up]
    fwd = bwd = kv
    blocks = [kv]
    state = None
    for step in range(1, n_sp // 2 + 1):
        nxt_f = lax.ppermute(fwd, "sp", up)
        nxt_b = lax.ppermute(bwd, "sp", down) if step < n_sp // 2 else None
        state = flash(qt, lift, blocks, state, block_rows, False)
        if step == 5:
            nxt_f, nxt_b, state, w_rows = lax.optimization_barrier((nxt_f, nxt_b, state, w_rows))
        else:
            nxt_f, nxt_b, state = lax.optimization_barrier((nxt_f, nxt_b, state))
        fwd, bwd = nxt_f, nxt_b
        blocks = [fwd] if bwd is None else [fwd, bwd]
    attended = flash(qt, lift, blocks, state, block_rows, True)
    w_rows = w_rows.reshape(NY, NXC, *w_rows.shape[1:])

    heads_y = lax.all_to_all(attended, "tp", 0, 0, axis_index_groups=group_y, tiled=True)
    part = out_partial(heads_y, w_rows)
    part = part.reshape(NXC, own_rows, width)
    parts = lax.all_to_all(part, "tp", 0, 0, axis_index_groups=group_cx, tiled=True)
    mixed = jnp.sum(parts.astype(jnp.float32), axis=0).astype(jnp.bfloat16)
    gate = mod[0, 2 * width :]
    return (latent.astype(jnp.float32) + gate * mixed.astype(jnp.float32)).astype(jnp.bfloat16)


def solution(mesh):
    return jax.shard_map(
        local,
        mesh=mesh,
        in_specs=(
            P(("sp", "tp"), None),
            P("sp", None),
            P("sp"),
            P("sp"),
            P("sp", "tp"),
            P(),
            P(None, "tp"),
            P(None, "tp"),
            P(None, "tp"),
            P(None, "tp"),
            P(),
            P(),
            P("tp"),
        ),
        out_specs=P(("sp", "tp"), None),
        check_vma=False,
    )
```

```python
import functools
import math
import jax
import jax.numpy as jnp
from jax import lax
from jax.experimental import pallas as pl
from jax.experimental.pallas import tpu as pltpu
from jax.sharding import PartitionSpec as P


GRID_W = 64
EPS = 1e-06
LOG2E = math.log2(math.e)
NY = 4
NX = 4
NXC = 8


def modulated(x, gain, shift):
    x = x.astype(jnp.float32)
    ms = jnp.mean(x * x, axis=-1, keepdims=True)
    return (x * lax.rsqrt(ms + EPS) * gain + shift).astype(jnp.bfloat16)


VMEM = pl.BlockSpec(memory_space=pltpu.VMEM)
SMEM = pl.BlockSpec(memory_space=pltpu.SMEM)


def near(*arrays):
    return [pltpu.with_memory_space_constraint(a, pltpu.VMEM) for a in arrays]


def spread_body(w_ref, o_ref, sems):
    copies = []
    for y in range(o_ref.shape[0]):
        for k in range(w_ref.shape[0]):
            copies.append(pltpu.make_async_copy(w_ref.at[k], o_ref.at[y, :, k], sems.at[y, k]))
    for copy in copies:
        copy.start()
    for copy in copies:
        copy.wait()


def spread(w):
    ny, nxc, kk, n = w.shape
    return pl.pallas_call(
        spread_body,
        in_specs=[VMEM],
        out_specs=pl.BlockSpec(memory_space=pl.ANY),
        out_shape=jax.ShapeDtypeStruct((ny, nxc, ny, kk, n), w.dtype),
        scratch_shapes=[pltpu.SemaphoreType.DMA((ny, ny))],
        cost_estimate=pl.CostEstimate(flops=0, bytes_accessed=10 * w.size, transcendentals=0),
        name="spread",
    )(w)


def qkv_body(hs, lat_ref, ctx_ref, gain_ref, shift_ref, wq_ref, wkv_ref, wq2_ref, wkv2_ref, qg_ref, kg_ref, cos_ref, sin_ref, own_ref, other_ref, ctx_kv_ref):
    def unit(v):
        return v * lax.rsqrt(jnp.mean(v * v, axis=-1, keepdims=True) + EPS)

    def turn(v, cos, sin):
        lane = lax.broadcasted_iota(jnp.int32, v.shape, 1)
        left = pltpu.roll(v, v.shape[1] - 1, 1)
        right = pltpu.roll(v, 1, 1)
        return v * cos + jnp.where(lane % 2 == 0, left, right) * sin

    def against(a, w):
        return lax.dot_general(a, w[...], (((1,), (1,)), ((), ())), preferred_element_type=jnp.float32)

    x = modulated(lat_ref[...], gain_ref[0:1], shift_ref[0:1])
    cos = cos_ref[...]
    sin = sin_ref[...]
    for wq, wkv, o_ref in ((wq_ref, wkv_ref, own_ref), (wq2_ref, wkv2_ref, other_ref)):
        y = jnp.dot(x, wq[...], preferred_element_type=jnp.float32)
        q = jnp.concatenate([unit(y[:, :hs]), unit(y[:, hs:])], axis=1) * qg_ref[...]
        q = turn(q, cos, sin).astype(jnp.bfloat16)
        o_ref[:, : 2 * hs] = q * jnp.bfloat16(hs ** -0.5)
        kv = against(x, wkv)
        k = unit(kv[:, :hs]) * kg_ref[...]
        k2 = turn(jnp.concatenate([k, k], axis=1), cos, sin)
        lane = lax.broadcasted_iota(jnp.int32, k2.shape, 1)
        o_ref[:, 2 * hs :] = jnp.where(lane < hs, k2, kv).astype(jnp.bfloat16)

    c = modulated(ctx_ref[...], gain_ref[1:2], shift_ref[1:2])
    ckv = against(c, wkv_ref)
    ck = unit(ckv[:, :hs]) * kg_ref[...]
    ctx_kv_ref[...] = jnp.concatenate([ck, ckv[:, hs:]], axis=1).astype(jnp.bfloat16)


def qkv(*args):
    rows = args[0].shape[0]
    n_ctx = args[1].shape[0]
    hs = args[9].shape[1]
    return pl.pallas_call(
        functools.partial(qkv_body, hs),
        in_specs=[VMEM] * len(args),
        out_specs=[VMEM] * 3,
        out_shape=[
            jax.ShapeDtypeStruct((rows, 4 * hs), jnp.bfloat16),
            jax.ShapeDtypeStruct((rows, 4 * hs), jnp.bfloat16),
            jax.ShapeDtypeStruct((n_ctx, 2 * hs), jnp.bfloat16),
        ],
        cost_estimate=pl.CostEstimate(
            flops=16 * rows * args[0].shape[1] * hs, bytes_accessed=6 << 20, transcendentals=0
        ),
        compiler_params=pltpu.CompilerParams(vmem_limit_bytes=24 << 20),
        name="qkv",
    )(*near(*args))


def assemble_body(core_ref, own_ref, got_ref, ctx_ref, qt_ref, kv_ref):
    rows = own_ref.shape[0]
    hs = qt_ref.shape[1]

    def put(ref, start):
        t = ref[:, : 2 * hs].astype(jnp.float32).T.astype(jnp.bfloat16)
        qt_ref[0, :, start : start + rows] = t[:hs]
        qt_ref[1, :, start : start + rows] = t[hs:]

    @pl.when(core_ref[0] == 0)
    def _():
        put(own_ref, 0)
        put(got_ref, rows)

    @pl.when(core_ref[0] != 0)
    def _():
        put(got_ref, 0)
        put(own_ref, rows)

    kv_ref[0:rows] = own_ref[:, 2 * hs :]
    kv_ref[rows : 2 * rows] = got_ref[:, 2 * hs :]
    kv_ref[2 * rows :] = ctx_ref[...]


def assemble(core, own, got, ctx_kv):
    rows, cols = own.shape
    hs = cols // 4
    return pl.pallas_call(
        assemble_body,
        in_specs=[SMEM, VMEM, VMEM, VMEM],
        out_specs=[VMEM, VMEM],
        out_shape=[
            pltpu.VMEM((2, hs, 2 * rows), jnp.bfloat16),
            pltpu.VMEM((2 * rows + ctx_kv.shape[0], 2 * hs), jnp.bfloat16),
        ],
        name="assemble",
    )(core, *near(own, got, ctx_kv))


def flash_body(n_blocks, first, last, lat_rows, hs, *refs):
    qt_ref, lift_ref = refs[:2]
    blocks = refs[2 : 2 + n_blocks]
    rest = refs[2 + n_blocks :]
    if not first:
        m_ref, l_ref, acc_ref = rest[:3]
        rest = rest[3:]
    heads, _, qn = qt_ref.shape
    lift = lift_ref[...]
    for h in range(heads):
        parts = []
        top = None
        for b in blocks:
            s = jnp.dot(b[:, :hs], qt_ref[h], preferred_element_type=jnp.float32) * LOG2E
            c = s[lat_rows:] + lift[h : h + 1] * LOG2E
            s = s[:lat_rows]
            t = jnp.maximum(jnp.max(s, axis=0, keepdims=True), jnp.max(c, axis=0, keepdims=True))
            top = t if top is None else jnp.maximum(top, t)
            parts.append((b, s, c))
        if first:
            l = jnp.zeros_like(top)
            acc = jnp.zeros((hs, qn), jnp.float32)
        else:
            m = m_ref[h : h + 1]
            top = jnp.maximum(top, m)
            alpha = jnp.exp2(m - top)
            l = l_ref[h : h + 1] * alpha
            acc = acc_ref[h] * alpha
        for b, s, c in parts:
            e = jnp.exp2(s - top)
            f = jnp.exp2(c - top)
            l = l + (jnp.sum(e, axis=0, keepdims=True) + jnp.sum(f, axis=0, keepdims=True))
            p = jnp.concatenate([e.astype(jnp.bfloat16), f.astype(jnp.bfloat16)], axis=0)
            acc = acc + lax.dot_general(
                b[:, hs:], p, (((0,), (0,)), ((), ())), preferred_element_type=jnp.float32
            )
        if last:
            o = (acc / l).T.astype(jnp.bfloat16)
            n = lat_rows // (2 * NY)
            for c2 in range(2):
                for y in range(NY):
                    j = (c2 * NY + y) * n
                    rest[0][y, c2 * n : (c2 + 1) * n, h * hs : (h + 1) * hs] = o[j : j + n]
        else:
            rest[0][h : h + 1] = top
            rest[1][h : h + 1] = l
            rest[2][h] = acc


def flash(qt, lift, blocks, state, lat_rows, last):
    heads, hs, qn = qt.shape
    first = state is None
    args = [qt, lift, *blocks] + ([] if first else list(state))
    args = near(*args)
    if last:
        outs = [pltpu.VMEM((NY, qn // NY, heads * hs), jnp.bfloat16)]
    else:
        outs = [
            pltpu.VMEM((heads, qn), jnp.float32),
            pltpu.VMEM((heads, qn), jnp.float32),
            pltpu.VMEM((heads, hs, qn), jnp.float32),
        ]
    res = pl.pallas_call(
        functools.partial(flash_body, len(blocks), first, last, lat_rows, hs),
        in_specs=[VMEM] * len(args),
        out_specs=[VMEM] * len(outs),
        out_shape=outs,
        cost_estimate=pl.CostEstimate(
            flops=4 * heads * hs * qn * blocks[0].shape[0] * len(blocks), bytes_accessed=1 << 20, transcendentals=0
        ),
        name="flash",
    )(*args)
    return res[0] if last else res


def project_body(core_ref, a_ref, w_ref, keep_ref, send_ref):
    ny = a_ref.shape[0]
    half = a_ref.shape[1] // 2
    core = core_ref[0]

    def rows_of(c):
        start = pl.multiple_of(c * half, half)
        return jnp.concatenate([a_ref[y, pl.ds(start, half), :] for y in range(ny)], axis=1)

    a = jnp.concatenate([rows_of(core), rows_of(1 - core)], axis=0)
    n = w_ref.shape[4]
    cols = [(i, j) for i in range(w_ref.shape[0]) for j in range(w_ref.shape[1])]

    def column(i, j):
        return jnp.concatenate([w_ref[i, j, y] for y in range(ny)], axis=0)

    for k in range(0, len(cols), 2):
        w = jnp.concatenate([column(*cols[k]), column(*cols[k + 1])], axis=1)
        r = jnp.dot(a, w, preferred_element_type=jnp.float32).astype(jnp.bfloat16)
        keep_ref[:, k * n : (k + 2) * n] = r[:half]
        send_ref[:, k * n : (k + 2) * n] = r[half:]


def out_partial(core, a, w):
    half = a.shape[1] // 2
    width = w.shape[0] * w.shape[1] * w.shape[4]
    return pl.pallas_call(
        project_body,
        in_specs=[SMEM, VMEM, VMEM],
        out_specs=[VMEM, VMEM],
        out_shape=[pltpu.VMEM((half, width), jnp.bfloat16), pltpu.VMEM((half, width), jnp.bfloat16)],
        cost_estimate=pl.CostEstimate(flops=4 * half * w.size, bytes_accessed=2 * w.size, transcendentals=0),
        compiler_params=pltpu.CompilerParams(vmem_limit_bytes=24 << 20),
        name="out_partial",
    )(core, *near(a, w))


def local(
    latent,
    context,
    condition,
    context_cond,
    mod_weight,
    norm_gain,
    query_weight,
    key_weight,
    value_weight,
    out_weight,
    query_gain,
    key_gain,
    context_lift,
):
    own_rows, width = latent.shape
    hs = query_gain.shape[0]
    n_sp = lax.axis_size("sp")
    n_tp = lax.axis_size("tp")
    group_y = [[y * NXC + c for y in range(NY)] for c in range(NXC)]
    group_x = [[y * NXC + 2 * x + c for x in range(NX)] for y in range(NY) for c in range(2)]
    group_core = [[2 * i + c for i in range(n_tp // 2)] for c in range(2)]
    swap = [(t, t ^ 1) for t in range(n_tp)]
    tp = lax.axis_index("tp")
    core = tp % 2
    block_rows = own_rows * n_tp

    lat_copies = jnp.broadcast_to(latent, (n_tp // 2, own_rows, width))
    lat_half = lax.all_to_all(lat_copies, "tp", 0, 0, axis_index_groups=group_core, tiled=True)
    lat_half = lat_half.reshape(block_rows // 2, width)

    half = jnp.arange(block_rows // 2, dtype=jnp.int32)
    inside = (half // own_rows) * (2 * own_rows) + core * own_rows + half % own_rows
    positions = lax.axis_index("sp") * block_rows + inside
    freq_count = hs // 4
    inverse = 10000.0 ** (-jnp.arange(freq_count, dtype=jnp.float32) / freq_count)
    grid_row = (positions // GRID_W).astype(jnp.float32)
    grid_col = (positions % GRID_W).astype(jnp.float32)
    angles = jnp.concatenate([grid_row[:, None] * inverse, grid_col[:, None] * inverse], axis=-1)
    cos = jnp.tile(jnp.repeat(jnp.cos(angles), 2, axis=1), (1, 2))
    sign = jnp.tile(jnp.array([-1.0, 1.0], jnp.float32), hs)
    sin = jnp.tile(jnp.repeat(jnp.sin(angles), 2, axis=1), (1, 2)) * sign
    lift = jnp.broadcast_to(context_lift[:, None], (context_lift.shape[0], block_rows))
    q_gain = jnp.tile(query_gain, 2)[None]
    k_gain = key_gain[None]

    cond_pair = jax.nn.silu(jnp.stack([condition, context_cond])).astype(jnp.bfloat16)
    partial_mod = jnp.dot(cond_pair, mod_weight, preferred_element_type=jnp.float32)
    run = math.gcd(n_sp, 4)
    near_z = [[g * run + i for i in range(run)] for g in range(n_sp // run)]
    far_z = [[g + run * i for i in range(n_sp // run)] for g in range(run)]
    summed_mod = lax.psum(lax.psum(partial_mod, "sp", axis_index_groups=near_z), "sp", axis_index_groups=far_z)
    summed_mod, lat_half, cos, sin, lift, q_gain, k_gain = lax.optimization_barrier(
        (summed_mod, lat_half, cos, sin, lift, q_gain, k_gain)
    )
    summed_mod, query_weight, key_weight, value_weight, out_weight = lax.optimization_barrier(
        (summed_mod, query_weight, key_weight, value_weight, out_weight)
    )
    wq = query_weight
    wkv = jnp.concatenate([key_weight.T, value_weight.T], axis=0)
    wq2 = lax.ppermute(wq, "tp", swap)
    wkv2 = lax.ppermute(wkv, "tp", swap)
    per_head = out_weight.shape[0] // n_tp
    w_split = spread(out_weight.reshape(NY, NXC, per_head, out_weight.shape[1]))
    w_split = w_split.reshape(n_tp, NY, per_head, out_weight.shape[1])
    mod_copies = jnp.broadcast_to(summed_mod, (n_tp, *summed_mod.shape))
    mod = lax.all_to_all(mod_copies, "tp", 0, 0, tiled=True)
    mod = jnp.moveaxis(mod, 0, 1).reshape(2, 3 * width)
    shift = mod[:, :width]
    gain = norm_gain * (1.0 + mod[:, width : 2 * width])

    own, other, ctx_kv = qkv(lat_half, context, gain, shift, wq, wkv, wq2, wkv2, q_gain, k_gain, cos, sin)
    got = lax.ppermute(other, "tp", swap)
    qt, kv = assemble(core.reshape(1).astype(jnp.int32), own, got, ctx_kv)
    kv, w_split = lax.optimization_barrier((kv, w_split))
    w_rows = lax.all_to_all(w_split, "tp", 0, 0, tiled=True)

    up = [(i, (i + 1) % n_sp) for i in range(n_sp)]
    down = [(d, s) for s, d in up]
    fwd = bwd = kv
    blocks = [kv]
    state = None
    for step in range(1, n_sp // 2 + 1):
        nxt_f = lax.ppermute(fwd, "sp", up)
        nxt_b = lax.ppermute(bwd, "sp", down) if step < n_sp // 2 else None
        state = flash(qt, lift, blocks, state, block_rows, False)
        if step == 7:
            nxt_f, nxt_b, state, w_rows = lax.optimization_barrier((nxt_f, nxt_b, state, w_rows))
        else:
            nxt_f, nxt_b, state = lax.optimization_barrier((nxt_f, nxt_b, state))
        fwd, bwd = nxt_f, nxt_b
        blocks = [fwd] if bwd is None else [fwd, bwd]
    attended = flash(qt, lift, blocks, state, block_rows, True)
    w_rows = w_rows.reshape(NY, NXC, *w_rows.shape[1:])

    heads_y = lax.all_to_all(attended, "tp", 0, 0, axis_index_groups=group_y, tiled=True)
    keep, send = out_partial(core.reshape(1).astype(jnp.int32), heads_y, w_rows)
    part = keep.astype(jnp.float32) + lax.ppermute(send, "tp", swap).astype(jnp.float32)
    part = part.astype(jnp.bfloat16).reshape(NX, own_rows, width)
    parts = lax.all_to_all(part, "tp", 0, 0, axis_index_groups=group_x, tiled=True)
    mixed = jnp.sum(parts.astype(jnp.float32), axis=0).astype(jnp.bfloat16)
    gate = mod[0, 2 * width :]
    return (latent.astype(jnp.float32) + gate * mixed.astype(jnp.float32)).astype(jnp.bfloat16)


def solution(mesh):
    return jax.shard_map(
        local,
        mesh=mesh,
        in_specs=(
            P(("sp", "tp"), None),
            P("sp", None),
            P("sp"),
            P("sp"),
            P("sp", "tp"),
            P(),
            P(None, "tp"),
            P(None, "tp"),
            P(None, "tp"),
            P(None, "tp"),
            P(),
            P(),
            P("tp"),
        ),
        out_specs=P(("sp", "tp"), None),
        check_vma=False,
    )
```

```python
import functools
import math
import jax
import jax.numpy as jnp
from jax import lax
from jax.experimental import pallas as pl
from jax.experimental.pallas import tpu as pltpu
from jax.sharding import PartitionSpec as P


GRID_W = 64
EPS = 1e-06
LOG2E = math.log2(math.e)
NY = 4
NX = 4
NXC = 8


def modulated(x, gain, shift):
    x = x.astype(jnp.float32)
    ms = jnp.mean(x * x, axis=-1, keepdims=True)
    return (x * lax.rsqrt(ms + EPS) * gain + shift).astype(jnp.bfloat16)


VMEM = pl.BlockSpec(memory_space=pltpu.VMEM)
SMEM = pl.BlockSpec(memory_space=pltpu.SMEM)


def near(*arrays):
    return [pltpu.with_memory_space_constraint(a, pltpu.VMEM) for a in arrays]


def spread_body(w_ref, o_ref, sems):
    copies = []
    for y in range(o_ref.shape[0]):
        for k in range(w_ref.shape[0]):
            copies.append(pltpu.make_async_copy(w_ref.at[k], o_ref.at[y, :, k], sems.at[y, k]))
    for copy in copies:
        copy.start()
    for copy in copies:
        copy.wait()


def spread(w):
    ny, nxc, kk, n = w.shape
    return pl.pallas_call(
        spread_body,
        in_specs=[VMEM],
        out_specs=pl.BlockSpec(memory_space=pl.ANY),
        out_shape=jax.ShapeDtypeStruct((ny, nxc, ny, kk, n), w.dtype),
        scratch_shapes=[pltpu.SemaphoreType.DMA((ny, ny))],
        cost_estimate=pl.CostEstimate(flops=0, bytes_accessed=10 * w.size, transcendentals=0),
        name="spread",
    )(w)


def repeat_body(x_ref, o_ref, sems):
    copies = [pltpu.make_async_copy(x_ref, o_ref.at[i], sems.at[i]) for i in range(o_ref.shape[0])]
    for copy in copies:
        copy.start()
    for copy in copies:
        copy.wait()


def repeated(x, count):
    return pl.pallas_call(
        repeat_body,
        in_specs=[VMEM],
        out_specs=pl.BlockSpec(memory_space=pl.ANY),
        out_shape=jax.ShapeDtypeStruct((count, *x.shape), x.dtype),
        scratch_shapes=[pltpu.SemaphoreType.DMA((count,))],
        cost_estimate=pl.CostEstimate(flops=0, bytes_accessed=2 * (count + 1) * x.size, transcendentals=0),
        name="repeated",
    )(x)


def qkv_body(hs, lat_ref, ctx_ref, gain_ref, shift_ref, wq_ref, wkv_ref, wq2_ref, wkv2_ref, qg_ref, kg_ref, cos_ref, sin_ref, own_ref, other_ref, ctx_kv_ref):
    def unit(v):
        return v * lax.rsqrt(jnp.mean(v * v, axis=-1, keepdims=True) + EPS)

    def turn(v, cos, sin):
        lane = lax.broadcasted_iota(jnp.int32, v.shape, 1)
        left = pltpu.roll(v, v.shape[1] - 1, 1)
        right = pltpu.roll(v, 1, 1)
        return v * cos + jnp.where(lane % 2 == 0, left, right) * sin

    def against(a, w):
        return lax.dot_general(a, w[...], (((1,), (1,)), ((), ())), preferred_element_type=jnp.float32)

    x = modulated(lat_ref[...], gain_ref[0:1], shift_ref[0:1])
    cos = cos_ref[...]
    sin = sin_ref[...]
    for wq, wkv, o_ref in ((wq_ref, wkv_ref, own_ref), (wq2_ref, wkv2_ref, other_ref)):
        y = jnp.dot(x, wq[...], preferred_element_type=jnp.float32)
        q = jnp.concatenate([unit(y[:, :hs]), unit(y[:, hs:])], axis=1) * qg_ref[...]
        q = turn(q, cos, sin).astype(jnp.bfloat16)
        o_ref[:, : 2 * hs] = q * jnp.bfloat16(hs ** -0.5)
        kv = against(x, wkv)
        k = unit(kv[:, :hs]) * kg_ref[...]
        k2 = turn(jnp.concatenate([k, k], axis=1), cos, sin)
        lane = lax.broadcasted_iota(jnp.int32, k2.shape, 1)
        o_ref[:, 2 * hs :] = jnp.where(lane < hs, k2, kv).astype(jnp.bfloat16)

    c = modulated(ctx_ref[...], gain_ref[1:2], shift_ref[1:2])
    ckv = against(c, wkv_ref)
    ck = unit(ckv[:, :hs]) * kg_ref[...]
    ctx_kv_ref[...] = jnp.concatenate([ck, ckv[:, hs:]], axis=1).astype(jnp.bfloat16)


def qkv(*args):
    rows = args[0].shape[0]
    n_ctx = args[1].shape[0]
    hs = args[9].shape[1]
    return pl.pallas_call(
        functools.partial(qkv_body, hs),
        in_specs=[VMEM] * len(args),
        out_specs=[VMEM] * 3,
        out_shape=[
            jax.ShapeDtypeStruct((rows, 4 * hs), jnp.bfloat16),
            jax.ShapeDtypeStruct((rows, 4 * hs), jnp.bfloat16),
            jax.ShapeDtypeStruct((n_ctx, 2 * hs), jnp.bfloat16),
        ],
        cost_estimate=pl.CostEstimate(
            flops=16 * rows * args[0].shape[1] * hs, bytes_accessed=6 << 20, transcendentals=0
        ),
        compiler_params=pltpu.CompilerParams(vmem_limit_bytes=24 << 20),
        name="qkv",
    )(*[near(a)[0] if a.size >= 1 << 19 else a for a in args])


def assemble_body(core_ref, own_ref, got_ref, ctx_ref, qt_ref, kv_ref):
    rows = own_ref.shape[0]
    hs = qt_ref.shape[1]

    def put(ref, start):
        t = ref[:, : 2 * hs].astype(jnp.float32).T.astype(jnp.bfloat16)
        qt_ref[0, :, start : start + rows] = t[:hs]
        qt_ref[1, :, start : start + rows] = t[hs:]

    @pl.when(core_ref[0] == 0)
    def _():
        put(own_ref, 0)
        put(got_ref, rows)

    @pl.when(core_ref[0] != 0)
    def _():
        put(got_ref, 0)
        put(own_ref, rows)

    kv_ref[0:rows] = own_ref[:, 2 * hs :]
    kv_ref[rows : 2 * rows] = got_ref[:, 2 * hs :]
    kv_ref[2 * rows :] = ctx_ref[...]


def assemble(core, own, got, ctx_kv):
    rows, cols = own.shape
    hs = cols // 4
    return pl.pallas_call(
        assemble_body,
        in_specs=[SMEM, VMEM, VMEM, VMEM],
        out_specs=[VMEM, VMEM],
        out_shape=[
            pltpu.VMEM((2, hs, 2 * rows), jnp.bfloat16),
            pltpu.VMEM((2 * rows + ctx_kv.shape[0], 2 * hs), jnp.bfloat16),
        ],
        name="assemble",
    )(core, *near(own, got, ctx_kv))


def flash_body(n_blocks, first, last, lat_rows, hs, *refs):
    qt_ref, lift_ref = refs[:2]
    blocks = refs[2 : 2 + n_blocks]
    rest = refs[2 + n_blocks :]
    if not first:
        m_ref, l_ref, acc_ref = rest[:3]
        rest = rest[3:]
    heads, _, qn = qt_ref.shape
    lift = lift_ref[...]
    for h in range(heads):
        parts = []
        top = None
        for b in blocks:
            s = jnp.dot(b[:, :hs], qt_ref[h], preferred_element_type=jnp.float32) * LOG2E
            c = s[lat_rows:] + lift[h : h + 1] * LOG2E
            s = s[:lat_rows]
            t = jnp.maximum(jnp.max(s, axis=0, keepdims=True), jnp.max(c, axis=0, keepdims=True))
            top = t if top is None else jnp.maximum(top, t)
            parts.append((b, s, c))
        if first:
            l = jnp.zeros_like(top)
            acc = jnp.zeros((hs, qn), jnp.float32)
        else:
            m = m_ref[h : h + 1]
            top = jnp.maximum(top, m)
            alpha = jnp.exp2(m - top)
            l = l_ref[h : h + 1] * alpha
            acc = acc_ref[h] * alpha
        for b, s, c in parts:
            e = jnp.exp2(s - top)
            f = jnp.exp2(c - top)
            l = l + (jnp.sum(e, axis=0, keepdims=True) + jnp.sum(f, axis=0, keepdims=True))
            p = jnp.concatenate([e.astype(jnp.bfloat16), f.astype(jnp.bfloat16)], axis=0)
            acc = acc + lax.dot_general(
                b[:, hs:], p, (((0,), (0,)), ((), ())), preferred_element_type=jnp.float32
            )
        if last:
            o = (acc / l).T.astype(jnp.bfloat16)
            n = lat_rows // (2 * NY)
            for c2 in range(2):
                for y in range(NY):
                    j = (c2 * NY + y) * n
                    rest[0][y, c2 * n : (c2 + 1) * n, h * hs : (h + 1) * hs] = o[j : j + n]
        else:
            rest[0][h : h + 1] = top
            rest[1][h : h + 1] = l
            rest[2][h] = acc


def flash(qt, lift, blocks, state, lat_rows, last):
    heads, hs, qn = qt.shape
    first = state is None
    args = [qt, lift, *blocks] + ([] if first else list(state))
    args = near(*args)
    if last:
        outs = [pltpu.VMEM((NY, qn // NY, heads * hs), jnp.bfloat16)]
    else:
        outs = [
            pltpu.VMEM((heads, qn), jnp.float32),
            pltpu.VMEM((heads, qn), jnp.float32),
            pltpu.VMEM((heads, hs, qn), jnp.float32),
        ]
    res = pl.pallas_call(
        functools.partial(flash_body, len(blocks), first, last, lat_rows, hs),
        in_specs=[VMEM] * len(args),
        out_specs=[VMEM] * len(outs),
        out_shape=outs,
        cost_estimate=pl.CostEstimate(
            flops=4 * heads * hs * qn * blocks[0].shape[0] * len(blocks), bytes_accessed=1 << 20, transcendentals=0
        ),
        name="flash",
    )(*args)
    return res[0] if last else res


def project_body(core_ref, a_ref, w_ref, keep_ref, send_ref):
    ny = a_ref.shape[0]
    half = a_ref.shape[1] // 2
    core = core_ref[0]

    def rows_of(c):
        start = pl.multiple_of(c * half, half)
        return jnp.concatenate([a_ref[y, pl.ds(start, half), :] for y in range(ny)], axis=1)

    a = jnp.concatenate([rows_of(core), rows_of(1 - core)], axis=0)
    n = w_ref.shape[4]
    cols = [(i, j) for i in range(w_ref.shape[0]) for j in range(w_ref.shape[1])]

    def column(i, j):
        return jnp.concatenate([w_ref[i, j, y] for y in range(ny)], axis=0)

    for k in range(0, len(cols), 2):
        w = jnp.concatenate([column(*cols[k]), column(*cols[k + 1])], axis=1)
        r = jnp.dot(a, w, preferred_element_type=jnp.float32).astype(jnp.bfloat16)
        keep_ref[:, k * n : (k + 2) * n] = r[:half]
        send_ref[:, k * n : (k + 2) * n] = r[half:]


def out_partial(core, a, w):
    half = a.shape[1] // 2
    width = w.shape[0] * w.shape[1] * w.shape[4]
    return pl.pallas_call(
        project_body,
        in_specs=[SMEM, VMEM, VMEM],
        out_specs=[VMEM, VMEM],
        out_shape=[pltpu.VMEM((half, width), jnp.bfloat16), pltpu.VMEM((half, width), jnp.bfloat16)],
        cost_estimate=pl.CostEstimate(flops=4 * half * w.size, bytes_accessed=2 * w.size, transcendentals=0),
        compiler_params=pltpu.CompilerParams(vmem_limit_bytes=24 << 20),
        name="out_partial",
    )(core, *near(a, w))


def local(
    latent,
    context,
    condition,
    context_cond,
    mod_weight,
    norm_gain,
    query_weight,
    key_weight,
    value_weight,
    out_weight,
    query_gain,
    key_gain,
    context_lift,
):
    own_rows, width = latent.shape
    hs = query_gain.shape[0]
    n_sp = lax.axis_size("sp")
    n_tp = lax.axis_size("tp")
    group_y = [[y * NXC + c for y in range(NY)] for c in range(NXC)]
    group_x = [[y * NXC + 2 * x + c for x in range(NX)] for y in range(NY) for c in range(2)]
    group_core = [[2 * i + c for i in range(n_tp // 2)] for c in range(2)]
    swap = [(t, t ^ 1) for t in range(n_tp)]
    tp = lax.axis_index("tp")
    core = tp % 2
    block_rows = own_rows * n_tp

    lat_copies = repeated(latent, n_tp // 2)
    lat_half = lax.all_to_all(lat_copies, "tp", 0, 0, axis_index_groups=group_core, tiled=True)
    lat_half = lat_half.reshape(block_rows // 2, width)

    half = jnp.arange(block_rows // 2, dtype=jnp.int32)
    inside = (half // own_rows) * (2 * own_rows) + core * own_rows + half % own_rows
    positions = lax.axis_index("sp") * block_rows + inside
    freq_count = hs // 4
    inverse = 10000.0 ** (-jnp.arange(freq_count, dtype=jnp.float32) / freq_count)
    grid_row = (positions // GRID_W).astype(jnp.float32)
    grid_col = (positions % GRID_W).astype(jnp.float32)
    angles = jnp.concatenate([grid_row[:, None] * inverse, grid_col[:, None] * inverse], axis=-1)
    cos = jnp.tile(jnp.repeat(jnp.cos(angles), 2, axis=1), (1, 2))
    sign = jnp.tile(jnp.array([-1.0, 1.0], jnp.float32), hs)
    sin = jnp.tile(jnp.repeat(jnp.sin(angles), 2, axis=1), (1, 2)) * sign
    lift = jnp.broadcast_to(context_lift[:, None], (context_lift.shape[0], block_rows))
    q_gain = jnp.tile(query_gain, 2)[None]
    k_gain = key_gain[None]

    cond_pair = jax.nn.silu(jnp.stack([condition, context_cond])).astype(jnp.bfloat16)
    partial_mod = jnp.dot(cond_pair, mod_weight, preferred_element_type=jnp.float32)
    run = math.gcd(n_sp, 4)
    near_z = [[g * run + i for i in range(run)] for g in range(n_sp // run)]
    far_z = [[g + run * i for i in range(n_sp // run)] for g in range(run)]
    summed_mod = lax.psum(lax.psum(partial_mod, "sp", axis_index_groups=near_z), "sp", axis_index_groups=far_z)
    summed_mod, lat_half, cos, sin, lift, q_gain, k_gain = lax.optimization_barrier(
        (summed_mod, lat_half, cos, sin, lift, q_gain, k_gain)
    )
    summed_mod, query_weight, key_weight, value_weight, out_weight = lax.optimization_barrier(
        (summed_mod, query_weight, key_weight, value_weight, out_weight)
    )
    wq = query_weight
    wkv = jnp.concatenate([key_weight.T, value_weight.T], axis=0)
    wq2 = lax.ppermute(wq, "tp", swap)
    wkv2 = lax.ppermute(wkv, "tp", swap)
    per_head = out_weight.shape[0] // n_tp
    w_split = spread(out_weight.reshape(NY, NXC, per_head, out_weight.shape[1]))
    w_split = w_split.reshape(n_tp, NY, per_head, out_weight.shape[1])
    mod_copies = jnp.broadcast_to(summed_mod, (n_tp, *summed_mod.shape))
    mod = lax.all_to_all(mod_copies, "tp", 0, 0, tiled=True)
    mod = jnp.moveaxis(mod, 0, 1).reshape(2, 3 * width)
    shift = mod[:, :width]
    gain = norm_gain * (1.0 + mod[:, width : 2 * width])

    own, other, ctx_kv = qkv(lat_half, context, gain, shift, wq, wkv, wq2, wkv2, q_gain, k_gain, cos, sin)
    got = lax.ppermute(other, "tp", swap)
    qt, kv = assemble(core.reshape(1).astype(jnp.int32), own, got, ctx_kv)

    up = [(i, (i + 1) % n_sp) for i in range(n_sp)]
    down = [(d, s) for s, d in up]
    fwd = bwd = kv
    blocks = [kv]
    state = None
    for step in range(1, n_sp // 2 + 1):
        nxt_f = lax.ppermute(fwd, "sp", up)
        nxt_b = lax.ppermute(bwd, "sp", down) if step < n_sp // 2 else None
        state = flash(qt, lift, blocks, state, block_rows, False)
        if step == 1:
            state, w_split = lax.optimization_barrier((state, w_split))
            w_rows = lax.all_to_all(w_split, "tp", 0, 0, tiled=True)
        if step == 7:
            nxt_f, nxt_b, state, w_rows = lax.optimization_barrier((nxt_f, nxt_b, state, w_rows))
        else:
            nxt_f, nxt_b, state = lax.optimization_barrier((nxt_f, nxt_b, state))
        fwd, bwd = nxt_f, nxt_b
        blocks = [fwd] if bwd is None else [fwd, bwd]
    attended = flash(qt, lift, blocks, state, block_rows, True)
    w_rows = w_rows.reshape(NY, NXC, *w_rows.shape[1:])

    heads_y = lax.all_to_all(attended, "tp", 0, 0, axis_index_groups=group_y, tiled=True)
    keep, send = out_partial(core.reshape(1).astype(jnp.int32), heads_y, w_rows)
    part = keep.astype(jnp.float32) + lax.ppermute(send, "tp", swap).astype(jnp.float32)
    part = part.astype(jnp.bfloat16).reshape(NX, own_rows, width)
    parts = lax.all_to_all(part, "tp", 0, 0, axis_index_groups=group_x, tiled=True)
    mixed = jnp.sum(parts.astype(jnp.float32), axis=0).astype(jnp.bfloat16)
    gate = mod[0, 2 * width :]
    return (latent.astype(jnp.float32) + gate * mixed.astype(jnp.float32)).astype(jnp.bfloat16)


def solution(mesh):
    return jax.shard_map(
        local,
        mesh=mesh,
        in_specs=(
            P(("sp", "tp"), None),
            P("sp", None),
            P("sp"),
            P("sp"),
            P("sp", "tp"),
            P(),
            P(None, "tp"),
            P(None, "tp"),
            P(None, "tp"),
            P(None, "tp"),
            P(),
            P(),
            P("tp"),
        ),
        out_specs=P(("sp", "tp"), None),
        check_vma=False,
    )
```

```python
import functools
import math
import jax
import jax.numpy as jnp
from jax import lax
from jax.experimental import pallas as pl
from jax.experimental.pallas import tpu as pltpu
from jax.sharding import PartitionSpec as P


GRID_W = 64
EPS = 1e-06
LOG2E = math.log2(math.e)
NY = 4
NX = 4
NXC = 8


def modulated(x, gain, shift):
    x = x.astype(jnp.float32)
    ms = jnp.mean(x * x, axis=-1, keepdims=True)
    return (x * lax.rsqrt(ms + EPS) * gain + shift).astype(jnp.bfloat16)


VMEM = pl.BlockSpec(memory_space=pltpu.VMEM)
SMEM = pl.BlockSpec(memory_space=pltpu.SMEM)


def near(*arrays):
    return [pltpu.with_memory_space_constraint(a, pltpu.VMEM) for a in arrays]


def spread_body(w_ref, o_ref, sems):
    copies = []
    for y in range(o_ref.shape[0]):
        for k in range(w_ref.shape[0]):
            copies.append(pltpu.make_async_copy(w_ref.at[k], o_ref.at[y, :, k], sems.at[y, k]))
    for copy in copies:
        copy.start()
    for copy in copies:
        copy.wait()


def spread(w):
    ny, nxc, kk, n = w.shape
    return pl.pallas_call(
        spread_body,
        in_specs=[VMEM],
        out_specs=pl.BlockSpec(memory_space=pl.ANY),
        out_shape=jax.ShapeDtypeStruct((ny, nxc, ny, kk, n), w.dtype),
        scratch_shapes=[pltpu.SemaphoreType.DMA((ny, ny))],
        cost_estimate=pl.CostEstimate(flops=0, bytes_accessed=10 * w.size, transcendentals=0),
        name="spread",
    )(w)


def repeat_body(x_ref, o_ref, sems):
    copies = [pltpu.make_async_copy(x_ref, o_ref.at[i], sems.at[i]) for i in range(o_ref.shape[0])]
    for copy in copies:
        copy.start()
    for copy in copies:
        copy.wait()


def repeated(x, count):
    return pl.pallas_call(
        repeat_body,
        in_specs=[VMEM],
        out_specs=pl.BlockSpec(memory_space=pl.ANY),
        out_shape=jax.ShapeDtypeStruct((count, *x.shape), x.dtype),
        scratch_shapes=[pltpu.SemaphoreType.DMA((count,))],
        cost_estimate=pl.CostEstimate(flops=0, bytes_accessed=2 * (count + 1) * x.size, transcendentals=0),
        name="repeated",
    )(x)


def qkv_body(hs, lat_ref, ctx_ref, gain_ref, shift_ref, wq_ref, wkv_ref, wq2_ref, wkv2_ref, qg_ref, kg_ref, cos_ref, sin_ref, own_ref, other_ref, ctx_kv_ref):
    def unit(v):
        return v * lax.rsqrt(jnp.mean(v * v, axis=-1, keepdims=True) + EPS)

    def turn(v, cos, sin):
        lane = lax.broadcasted_iota(jnp.int32, v.shape, 1)
        left = pltpu.roll(v, v.shape[1] - 1, 1)
        right = pltpu.roll(v, 1, 1)
        return v * cos + jnp.where(lane % 2 == 0, left, right) * sin

    def against(a, w):
        return lax.dot_general(a, w[...], (((1,), (1,)), ((), ())), preferred_element_type=jnp.float32)

    x = modulated(lat_ref[...], gain_ref[0:1], shift_ref[0:1])
    cos = cos_ref[...]
    sin = sin_ref[...]
    for wq, wkv, o_ref in ((wq_ref, wkv_ref, own_ref), (wq2_ref, wkv2_ref, other_ref)):
        y = jnp.dot(x, wq[...], preferred_element_type=jnp.float32)
        q = jnp.concatenate([unit(y[:, :hs]), unit(y[:, hs:])], axis=1) * qg_ref[...]
        q = turn(q, cos, sin).astype(jnp.bfloat16)
        o_ref[:, : 2 * hs] = q * jnp.bfloat16(hs ** -0.5)
        kv = against(x, wkv)
        k = unit(kv[:, :hs]) * kg_ref[...]
        k2 = turn(jnp.concatenate([k, k], axis=1), cos, sin)
        lane = lax.broadcasted_iota(jnp.int32, k2.shape, 1)
        o_ref[:, 2 * hs :] = jnp.where(lane < hs, k2, kv).astype(jnp.bfloat16)

    c = modulated(ctx_ref[...], gain_ref[1:2], shift_ref[1:2])
    ckv = against(c, wkv_ref)
    ck = unit(ckv[:, :hs]) * kg_ref[...]
    ctx_kv_ref[...] = jnp.concatenate([ck, ckv[:, hs:]], axis=1).astype(jnp.bfloat16)


def qkv(*args):
    rows = args[0].shape[0]
    n_ctx = args[1].shape[0]
    hs = args[9].shape[1]
    return pl.pallas_call(
        functools.partial(qkv_body, hs),
        in_specs=[VMEM] * len(args),
        out_specs=[VMEM] * 3,
        out_shape=[
            jax.ShapeDtypeStruct((rows, 4 * hs), jnp.bfloat16),
            jax.ShapeDtypeStruct((rows, 4 * hs), jnp.bfloat16),
            jax.ShapeDtypeStruct((n_ctx, 2 * hs), jnp.bfloat16),
        ],
        cost_estimate=pl.CostEstimate(
            flops=16 * rows * args[0].shape[1] * hs, bytes_accessed=6 << 20, transcendentals=0
        ),
        compiler_params=pltpu.CompilerParams(vmem_limit_bytes=24 << 20),
        name="qkv",
    )(*[near(a)[0] if a.size >= 1 << 19 else a for a in args])


def assemble_body(core_ref, own_ref, got_ref, ctx_ref, qt_ref, kv_ref):
    rows = own_ref.shape[0]
    hs = qt_ref.shape[1]

    def put(ref, start):
        t = ref[:, : 2 * hs].astype(jnp.float32).T.astype(jnp.bfloat16)
        qt_ref[0, :, start : start + rows] = t[:hs]
        qt_ref[1, :, start : start + rows] = t[hs:]

    @pl.when(core_ref[0] == 0)
    def _():
        put(own_ref, 0)
        put(got_ref, rows)

    @pl.when(core_ref[0] != 0)
    def _():
        put(got_ref, 0)
        put(own_ref, rows)

    kv_ref[0:rows] = own_ref[:, 2 * hs :]
    kv_ref[rows : 2 * rows] = got_ref[:, 2 * hs :]
    kv_ref[2 * rows :] = ctx_ref[...]


def assemble(core, own, got, ctx_kv):
    rows, cols = own.shape
    hs = cols // 4
    return pl.pallas_call(
        assemble_body,
        in_specs=[SMEM, VMEM, VMEM, VMEM],
        out_specs=[VMEM, VMEM],
        out_shape=[
            pltpu.VMEM((2, hs, 2 * rows), jnp.bfloat16),
            pltpu.VMEM((2 * rows + ctx_kv.shape[0], 2 * hs), jnp.bfloat16),
        ],
        name="assemble",
    )(core, *near(own, got, ctx_kv))


def flash_body(n_blocks, first, last, lat_rows, hs, *refs):
    qt_ref, lift_ref = refs[:2]
    blocks = refs[2 : 2 + n_blocks]
    rest = refs[2 + n_blocks :]
    if not first:
        m_ref, l_ref, acc_ref = rest[:3]
        rest = rest[3:]
    heads, _, qn = qt_ref.shape
    lift = lift_ref[...]
    for h in range(heads):
        parts = []
        top = None
        for b in blocks:
            s = jnp.dot(b[:, :hs], qt_ref[h], preferred_element_type=jnp.float32) * LOG2E
            c = s[lat_rows:] + lift[h : h + 1] * LOG2E
            s = s[:lat_rows]
            t = jnp.maximum(jnp.max(s, axis=0, keepdims=True), jnp.max(c, axis=0, keepdims=True))
            top = t if top is None else jnp.maximum(top, t)
            parts.append((b, s, c))
        if first:
            l = jnp.zeros_like(top)
            acc = jnp.zeros((hs, qn), jnp.float32)
        else:
            m = m_ref[h : h + 1]
            top = jnp.maximum(top, m)
            alpha = jnp.exp2(m - top)
            l = l_ref[h : h + 1] * alpha
            acc = acc_ref[h] * alpha
        for b, s, c in parts:
            e = jnp.exp2(s - top)
            f = jnp.exp2(c - top)
            l = l + (jnp.sum(e, axis=0, keepdims=True) + jnp.sum(f, axis=0, keepdims=True))
            p = jnp.concatenate([e.astype(jnp.bfloat16), f.astype(jnp.bfloat16)], axis=0)
            acc = acc + lax.dot_general(
                b[:, hs:], p, (((0,), (0,)), ((), ())), preferred_element_type=jnp.float32
            )
        if last:
            o = (acc / l).T.astype(jnp.bfloat16)
            n = lat_rows // (2 * NY)
            for c2 in range(2):
                for y in range(NY):
                    j = (c2 * NY + y) * n
                    rest[0][y, c2 * n : (c2 + 1) * n, h * hs : (h + 1) * hs] = o[j : j + n]
        else:
            rest[0][h : h + 1] = top
            rest[1][h : h + 1] = l
            rest[2][h] = acc


def flash(qt, lift, blocks, state, lat_rows, last):
    heads, hs, qn = qt.shape
    first = state is None
    args = [qt, lift, *blocks] + ([] if first else list(state))
    args = near(*args)
    if last:
        outs = [pltpu.VMEM((NY, qn // NY, heads * hs), jnp.bfloat16)]
    else:
        outs = [
            pltpu.VMEM((heads, qn), jnp.float32),
            pltpu.VMEM((heads, qn), jnp.float32),
            pltpu.VMEM((heads, hs, qn), jnp.float32),
        ]
    res = pl.pallas_call(
        functools.partial(flash_body, len(blocks), first, last, lat_rows, hs),
        in_specs=[VMEM] * len(args),
        out_specs=[VMEM] * len(outs),
        out_shape=outs,
        cost_estimate=pl.CostEstimate(
            flops=4 * heads * hs * qn * blocks[0].shape[0] * len(blocks), bytes_accessed=1 << 20, transcendentals=0
        ),
        name="flash",
    )(*args)
    return res[0] if last else res


def project_body(core_ref, a_ref, w_ref, keep_ref, send_ref):
    ny = a_ref.shape[0]
    half = a_ref.shape[1] // 2
    core = core_ref[0]

    def rows_of(c):
        start = pl.multiple_of(c * half, half)
        return jnp.concatenate([a_ref[y, pl.ds(start, half), :] for y in range(ny)], axis=1)

    a = jnp.concatenate([rows_of(core), rows_of(1 - core)], axis=0)
    n = w_ref.shape[4]
    cols = [(i, j) for i in range(w_ref.shape[0]) for j in range(w_ref.shape[1])]

    def column(i, j):
        return jnp.concatenate([w_ref[i, j, y] for y in range(ny)], axis=0)

    for k in range(0, len(cols), 2):
        w = jnp.concatenate([column(*cols[k]), column(*cols[k + 1])], axis=1)
        r = jnp.dot(a, w, preferred_element_type=jnp.float32).astype(jnp.bfloat16)
        keep_ref[:, k * n : (k + 2) * n] = r[:half]
        send_ref[:, k * n : (k + 2) * n] = r[half:]


def out_partial(core, a, w):
    half = a.shape[1] // 2
    width = w.shape[0] * w.shape[1] * w.shape[4]
    return pl.pallas_call(
        project_body,
        in_specs=[SMEM, VMEM, VMEM],
        out_specs=[VMEM, VMEM],
        out_shape=[pltpu.VMEM((half, width), jnp.bfloat16), pltpu.VMEM((half, width), jnp.bfloat16)],
        cost_estimate=pl.CostEstimate(flops=4 * half * w.size, bytes_accessed=2 * w.size, transcendentals=0),
        compiler_params=pltpu.CompilerParams(vmem_limit_bytes=24 << 20),
        name="out_partial",
    )(core, *near(a, w))


def local(
    latent,
    context,
    condition,
    context_cond,
    mod_weight,
    norm_gain,
    query_weight,
    key_weight,
    value_weight,
    out_weight,
    query_gain,
    key_gain,
    context_lift,
):
    own_rows, width = latent.shape
    hs = query_gain.shape[0]
    n_sp = lax.axis_size("sp")
    n_tp = lax.axis_size("tp")
    group_y = [[y * NXC + c for y in range(NY)] for c in range(NXC)]
    group_x = [[y * NXC + 2 * x + c for x in range(NX)] for y in range(NY) for c in range(2)]
    group_core = [[2 * i + c for i in range(n_tp // 2)] for c in range(2)]
    swap = [(t, t ^ 1) for t in range(n_tp)]
    tp = lax.axis_index("tp")
    core = tp % 2
    block_rows = own_rows * n_tp

    lat_copies = repeated(latent, n_tp // 2)
    lat_half = lax.all_to_all(lat_copies, "tp", 0, 0, axis_index_groups=group_core, tiled=True)
    lat_half = lat_half.reshape(block_rows // 2, width)

    half = jnp.arange(block_rows // 2, dtype=jnp.int32)
    inside = (half // own_rows) * (2 * own_rows) + core * own_rows + half % own_rows
    positions = lax.axis_index("sp") * block_rows + inside
    freq_count = hs // 4
    lane = lax.broadcasted_iota(jnp.int32, (block_rows // 2, 2 * hs), 1)
    pair = lane % hs // 2
    inverse = 10000.0 ** (-(pair % freq_count).astype(jnp.float32) / freq_count)
    along = jnp.where(pair < freq_count, positions[:, None] // GRID_W, positions[:, None] % GRID_W)
    angles = along.astype(jnp.float32) * inverse
    cos = jnp.cos(angles)
    sin = jnp.where(lane % 2 == 0, -jnp.sin(angles), jnp.sin(angles))
    lift = jnp.broadcast_to(context_lift[:, None], (context_lift.shape[0], block_rows))
    q_gain = jnp.tile(query_gain, 2)[None]
    k_gain = key_gain[None]

    cond_pair = jax.nn.silu(jnp.stack([condition, context_cond])).astype(jnp.bfloat16)
    partial_mod = jnp.dot(cond_pair, mod_weight, preferred_element_type=jnp.float32)
    run = math.gcd(n_sp, 4)
    near_z = [[g * run + i for i in range(run)] for g in range(n_sp // run)]
    far_z = [[g + run * i for i in range(n_sp // run)] for g in range(run)]
    summed_mod = lax.psum(lax.psum(partial_mod, "sp", axis_index_groups=near_z), "sp", axis_index_groups=far_z)
    summed_mod, lat_half, cos, sin, lift, q_gain, k_gain = lax.optimization_barrier(
        (summed_mod, lat_half, cos, sin, lift, q_gain, k_gain)
    )
    summed_mod, query_weight, key_weight, value_weight, out_weight = lax.optimization_barrier(
        (summed_mod, query_weight, key_weight, value_weight, out_weight)
    )
    wq = query_weight
    wkv = jnp.concatenate([key_weight.T, value_weight.T], axis=0)
    wq2 = lax.ppermute(wq, "tp", swap)
    wkv2 = lax.ppermute(wkv, "tp", swap)
    per_head = out_weight.shape[0] // n_tp
    w_split = spread(out_weight.reshape(NY, NXC, per_head, out_weight.shape[1]))
    w_split = w_split.reshape(n_tp, NY, per_head, out_weight.shape[1])
    mod_copies = jnp.broadcast_to(summed_mod, (n_tp, *summed_mod.shape))
    mod = lax.all_to_all(mod_copies, "tp", 0, 0, tiled=True)
    mod = jnp.moveaxis(mod, 0, 1).reshape(2, 3 * width)
    shift = mod[:, :width]
    gain = norm_gain * (1.0 + mod[:, width : 2 * width])

    own, other, ctx_kv = qkv(lat_half, context, gain, shift, wq, wkv, wq2, wkv2, q_gain, k_gain, cos, sin)
    got = lax.ppermute(other, "tp", swap)
    qt, kv = assemble(core.reshape(1).astype(jnp.int32), own, got, ctx_kv)

    up = [(i, (i + 1) % n_sp) for i in range(n_sp)]
    down = [(d, s) for s, d in up]
    fwd = bwd = kv
    blocks = [kv]
    state = None
    for step in range(1, n_sp // 2 + 1):
        nxt_f = lax.ppermute(fwd, "sp", up)
        nxt_b = lax.ppermute(bwd, "sp", down) if step < n_sp // 2 else None
        state = flash(qt, lift, blocks, state, block_rows, False)
        if step == 1:
            state, w_split = lax.optimization_barrier((state, w_split))
            w_rows = lax.all_to_all(w_split, "tp", 0, 0, tiled=True)
        if step == 7:
            nxt_f, nxt_b, state, w_rows = lax.optimization_barrier((nxt_f, nxt_b, state, w_rows))
        else:
            nxt_f, nxt_b, state = lax.optimization_barrier((nxt_f, nxt_b, state))
        fwd, bwd = nxt_f, nxt_b
        blocks = [fwd] if bwd is None else [fwd, bwd]
    attended = flash(qt, lift, blocks, state, block_rows, True)
    w_rows = w_rows.reshape(NY, NXC, *w_rows.shape[1:])

    heads_y = lax.all_to_all(attended, "tp", 0, 0, axis_index_groups=group_y, tiled=True)
    keep, send = out_partial(core.reshape(1).astype(jnp.int32), heads_y, w_rows)
    part = keep.astype(jnp.float32) + lax.ppermute(send, "tp", swap).astype(jnp.float32)
    part = part.astype(jnp.bfloat16).reshape(NX, own_rows, width)
    parts = lax.all_to_all(part, "tp", 0, 0, axis_index_groups=group_x, tiled=True)
    mixed = jnp.sum(parts.astype(jnp.float32), axis=0).astype(jnp.bfloat16)
    gate = mod[0, 2 * width :]
    return (latent.astype(jnp.float32) + gate * mixed.astype(jnp.float32)).astype(jnp.bfloat16)


def solution(mesh):
    return jax.shard_map(
        local,
        mesh=mesh,
        in_specs=(
            P(("sp", "tp"), None),
            P("sp", None),
            P("sp"),
            P("sp"),
            P("sp", "tp"),
            P(),
            P(None, "tp"),
            P(None, "tp"),
            P(None, "tp"),
            P(None, "tp"),
            P(),
            P(),
            P("tp"),
        ),
        out_specs=P(("sp", "tp"), None),
        check_vma=False,
    )
```
